32 devices in a mesh: sp: 8 (over z, y), tp: 4 (over x, core).
Axes of the slice: x: 2, y: 2, z: 4, core: 2. Of those that a mesh axis runs over, the one named last changes fastest.
Arguments:
- layer_input: bfloat16 [6144, 2048], P('sp', 'tp'), may hold values from -6 to 6
- input_norm_gain: bfloat16 [2048], replicated, may hold values from 0.099609375 to 1.8984375
- query_weight: bfloat16 [2048, 2048], P(None, 'tp'), may hold values from -0.125 to 0.125
- forget_weight: bfloat16 [2048, 2048], P(None, 'tp'), may hold values from -0.125 to 0.125
- value_matrix: bfloat16 [2048, 2048], P(None, 'tp'), may hold values from -0.125 to 0.125
- output_gate_weight: bfloat16 [2048, 2048], P(None, 'tp'), may hold values from -0.125 to 0.125
- after_gate_weight: bfloat16 [2048, 2048], P(None, 'tp'), may hold values from -0.125 to 0.125
- before_gate_weight: bfloat16 [2048, 2048], P(None, 'tp'), may hold values from -0.125 to 0.125
- convolution_input_weight: bfloat16 [2048, 2048], P(None, 'tp'), may hold values from -0.125 to 0.125
- forget_minimum: float32 [2048], P('tp'), may hold values from 0.95 to 0.9999837
- surge_log_decay: float32 [6144, 2048], P('sp', 'tp'), may hold values from -2.2 to 0
- convolution_kernel: bfloat16 [3, 2048], P(None, 'tp'), may hold values from -4 to 4
- head_norm_gain: bfloat16 [128], replicated, may hold values from 0.099609375 to 1.8984375
- starting_state: float32 [16, 128, 128], P('tp', 'sp'), may hold values from -0.09375 to 0.09375
- recurrence_output_weight: bfloat16 [2048, 2048], P('tp'), may hold values from -0.09375 to 0.09375
- convolution_output_weight: bfloat16 [2048, 2048], P('tp'), may hold values from -0.09375 to 0.09375
- output_norm_gain: bfloat16 [2048], replicated, may hold values from 0.099609375 to 1.8984375
Outputs:
- layer_out: bfloat16 [6144, 2048], P(('sp', 'tp'))
The draws below stay inside these ranges and needn't reach their ends.
All inputs are finite; a program needn't handle non-finite values.
Results may differ from the reference program's by a relative error of at most 0.014.
Values may be sent and summed in bfloat16 or wider, within the bound.
No kernel may reach another device: no remote copies, remote signals or barrier semaphores. Data moves between devices by JAX's collectives and lax.ppermute only.
A program may use at most 128 MiB of HBM per device.

```python
import jax
import jax.numpy as jnp
from jax import lax

D = 2048
HEADS = 16
DK = 128
DV = 128
CW = 2048
CK = 3
BLK = 64
TOKENS_PER_SHARD = 768
TOKENS = 6144
KEYW = 2048
VALW = 2048


def decay_tables(key):
    keys = jax.random.split(jax.random.fold_in(key, 11), 6)
    share = 0.5
    slow_head = jax.random.uniform(keys[0], (HEADS,), jnp.float32) < share
    slow = jnp.repeat(slow_head, DK)
    rate = jnp.exp(jax.random.uniform(keys[1], (HEADS * DK,), jnp.float32, jnp.log(0.1), jnp.log(0.6))) / TOKENS
    fast_floor = jax.random.uniform(keys[2], (HEADS * DK,), jnp.float32, 0.95, 0.99)
    forget_minimum = jnp.where(slow, 1.0 - rate, fast_floor)
    extra_decay = jnp.where(slow, rate, 0.03)
    decay_factor = jnp.exp(jax.random.uniform(keys[3], (TOKENS // TOKENS_PER_SHARD,), jnp.float32, jnp.log(0.5), jnp.log(2.0)))
    spots = jax.random.randint(keys[4], (3,), 0, TOKENS)
    losses = jnp.log(jax.random.uniform(keys[5], (3,), jnp.float32, 0.5, 0.8))
    position = jnp.arange(TOKENS)
    decay_surge = jnp.sum(jnp.where(position[:, None] == spots[None, :], losses[None, :], 0.0), axis=1)
    surge_log_decay = -jnp.repeat(decay_factor, TOKENS_PER_SHARD)[:, None] * extra_decay[None, :] + decay_surge[:, None]
    return (forget_minimum.astype(jnp.float32), surge_log_decay.astype(jnp.float32))


def draw_forget_minimum(key, part):
    return decay_tables(key)[0]


def draw_surge_log_decay(key, part):
    return decay_tables(key)[1]


def shard_levels(key, shape, pieces, least, largest):
    factor_of, own = 1.0, jax.random.fold_in(key, 6)
    for dim, blocks in pieces:
        draws = jnp.exp(jax.random.uniform(jax.random.fold_in(own, dim), (blocks,), jnp.float32, least / len(pieces), largest / len(pieces)))
        factor_of = factor_of * jnp.repeat(draws, shape[dim] // blocks).reshape([-1 if axis == dim else 1 for axis in range(len(shape))])
    return factor_of


def normal_values(key, dims, deviation, limit, cuts=(), held_as=jnp.bfloat16):
    entries = jax.random.normal(key, dims, jnp.float32) * deviation
    if len(cuts) > 0:
        entries = shard_levels(key, dims, cuts, -0.22, 0.18) * entries
    return jnp.clip(entries, min=-limit, max=limit).astype(held_as)


def setup_inputs(seed: int = 0) -> dict:
    key_list = jax.random.split(jax.random.key(seed), 18)
    return {
        "layer_input": normal_values(key_list[0], (TOKENS, D), 1.0, 6.0, ((0, 8), (1, 4))),
        "input_norm_gain": jnp.clip(1.0 + 0.18 * jax.random.normal(key_list[1], (D,), jnp.float32), 0.099609375, 1.8984375).astype(jnp.bfloat16),
        "query_weight": normal_values(key_list[2], (D, KEYW), D ** -0.5, 0.125, ((1, 4),)),
        "forget_weight": normal_values(key_list[3], (D, KEYW), D ** -0.5, 0.125, ((1, 4),)),
        "value_matrix": normal_values(key_list[4], (D, VALW), D ** -0.5, 0.125, ((1, 4),)),
        "output_gate_weight": normal_values(key_list[5], (D, VALW), D ** -0.5, 0.125, ((1, 4),)),
        "after_gate_weight": normal_values(key_list[6], (D, CW), D ** -0.5, 0.125, ((1, 4),)),
        "before_gate_weight": normal_values(key_list[7], (D, CW), D ** -0.5, 0.125, ((1, 4),)),
        "convolution_input_weight": normal_values(key_list[8], (D, CW), D ** -0.5, 0.125, ((1, 4),)),
        "forget_minimum": draw_forget_minimum(jax.random.fold_in(key_list[17], 71), 0),
        "surge_log_decay": draw_surge_log_decay(jax.random.fold_in(key_list[17], 71), 0),
        "convolution_kernel": normal_values(key_list[11], (CK, CW), 0.577, 4.0, ((1, 4),)),
        "head_norm_gain": jnp.clip(1.0 + 0.18 * jax.random.normal(key_list[12], (DV,), jnp.float32), 0.099609375, 1.8984375).astype(jnp.bfloat16),
        "starting_state": normal_values(key_list[13], (HEADS, DK, DV), (0.5 * TOKENS ** -0.5), 0.09375, ((0, 4), (1, 8)), jnp.float32),
        "recurrence_output_weight": normal_values(key_list[14], (VALW, D), (VALW + CW) ** -0.5, 0.09375, ((0, 4),)),
        "convolution_output_weight": normal_values(key_list[15], (CW, D), (VALW + CW) ** -0.5, 0.09375, ((0, 4),)),
        "output_norm_gain": jnp.clip(1.0 + 0.18 * jax.random.normal(key_list[16], (D,), jnp.float32), 0.099609375, 1.8984375).astype(jnp.bfloat16),
    }


EPS = 1e-06
PRECISE_PRODUCT = lax.Precision.HIGHEST

def rms_scale(value_rows):
    return lax.rsqrt(lax.optimization_barrier(jnp.mean(value_rows * value_rows, axis=-1, keepdims=True)) + EPS)

def project(normed, weight):
    return jnp.dot(normed, weight, preferred_element_type=jnp.float32).astype(jnp.bfloat16)

def block_pass(latent_state, inputs):
    query_rows, key_inputs, value_rows, forget_gate_logits = inputs
    cumulative_decay = jnp.cumsum(forget_gate_logits, axis=1)
    length = query_rows.shape[1]
    causal_masking = jnp.tril(jnp.ones((length, length), dtype=bool))[None, :, :, None]
    crossed_output = jnp.einsum('rmq,rqu->rmu', query_rows * jnp.exp(cumulative_decay), latent_state, precision=PRECISE_PRODUCT)
    decay = jnp.exp(jnp.where(causal_masking, cumulative_decay[:, :, None, :] - cumulative_decay[:, None, :, :], -jnp.inf))
    scores = jnp.einsum('htk,hsk,htsk->hts', query_rows, key_inputs, decay, precision=PRECISE_PRODUCT)
    o_intra = jnp.einsum('hts,hsv->htv', scores, value_rows, precision=PRECISE_PRODUCT)
    final_state = cumulative_decay[:, -1:, :]
    latent_state = jnp.exp(final_state[:, 0, :])[..., None] * latent_state + jnp.einsum('xar,xai->xri', key_inputs * jnp.exp(final_state - cumulative_decay), value_rows, precision=PRECISE_PRODUCT)
    return (latent_state, o_intra + crossed_output)

def reference(layer_input, input_norm_gain, query_weight, forget_weight, value_matrix, output_gate_weight, after_gate_weight, before_gate_weight, convolution_input_weight, forget_minimum, surge_log_decay, convolution_kernel, head_norm_gain, starting_state, recurrence_output_weight, convolution_output_weight, output_norm_gain):
    rows_f = layer_input.astype(jnp.float32)
    normed = (rows_f * rms_scale(rows_f) * input_norm_gain.astype(jnp.float32)).astype(jnp.bfloat16)
    query_raw = project(normed, query_weight)
    forget_raw = project(normed, forget_weight)
    value_raw = project(normed, value_matrix)
    outgate_raw = project(normed, output_gate_weight)
    postgate_raw = project(normed, after_gate_weight)
    pregate_raw = project(normed, before_gate_weight)
    convval_raw = project(normed, convolution_input_weight)
    forget_single = forget_raw.astype(jnp.float32)
    forget_gate_logits = jnp.logaddexp(jnp.log(forget_minimum), jnp.log1p(-forget_minimum) + jax.nn.log_sigmoid(forget_single)) + surge_log_decay
    key_inputs = (1.0 - forget_minimum) * jax.nn.sigmoid(-forget_single)
    query_rows = jax.nn.silu(query_raw.astype(jnp.float32)) * DK ** (-0.5)
    blocks = TOKENS // BLK

    def to_blocks(value_rows, width):
        return value_rows.reshape(blocks, BLK, HEADS, width).transpose(0, 2, 1, 3)
    _, outputs = lax.scan(block_pass, starting_state.astype(jnp.float32), (to_blocks(query_rows, DK), to_blocks(key_inputs, DK), to_blocks(value_raw.astype(jnp.float32), DV), to_blocks(forget_gate_logits, DK)))
    recurrence_step = outputs.transpose(0, 2, 1, 3).reshape(TOKENS, HEADS, DV)
    normed_heads = recurrence_step * rms_scale(recurrence_step) * head_norm_gain.astype(jnp.float32)
    rec_out = (normed_heads.reshape(TOKENS, HEADS * DV) * jax.nn.silu(outgate_raw.astype(jnp.float32))).astype(jnp.bfloat16)
    mixed_in = pregate_raw.astype(jnp.float32) * convval_raw.astype(jnp.float32)
    padded = jnp.concatenate([jnp.zeros((CK - 1, mixed_in.shape[1]), jnp.float32), mixed_in], axis=0)
    taps_f = convolution_kernel.astype(jnp.float32)
    conv_sum = padded[0:TOKENS] * taps_f[0]
    for offset in range(1, CK):
        conv_sum = conv_sum + padded[offset:offset + TOKENS] * taps_f[offset]
    conv_out = (postgate_raw.astype(jnp.float32) * conv_sum).astype(jnp.bfloat16)
    mixed = jnp.dot(rec_out, recurrence_output_weight, preferred_element_type=jnp.float32) + jnp.dot(conv_out, convolution_output_weight, preferred_element_type=jnp.float32)
    return (mixed * rms_scale(mixed) * output_norm_gain.astype(jnp.float32)).astype(jnp.bfloat16)
```

```python
import functools

import jax
import jax.numpy as jnp
from jax import lax
from jax.experimental import pallas as pl
from jax.experimental.pallas import tpu as pltpu
from jax.sharding import PartitionSpec as P

DK = 128
DV = 128
CK = 3
EPS = 1e-06
F32 = jnp.float32
BF16 = jnp.bfloat16
ANY = pl.BlockSpec(memory_space=pl.ANY)
VMEM = pl.BlockSpec(memory_space=pltpu.VMEM)
SMEM = pl.BlockSpec(memory_space=pltpu.SMEM)


def xor_permute(value, axis, bit):
    peers = lax.axis_size(axis)
    return lax.ppermute(value, axis, [(i, i ^ bit) for i in range(peers)])


def from_behind(value, axis, by):
    peers = lax.axis_size(axis)
    return lax.ppermute(value, axis, [(i, i + by) for i in range(peers) if 0 <= i + by < peers])


def dot_nt(a, b):
    return lax.dot_general(a, b, (((1,), (1,)), ((), ())), preferred_element_type=F32)


def dot_tn(a, b):
    return lax.dot_general(a, b, (((0,), (0,)), ((), ())), preferred_element_type=F32)


def state_kernel(pieces, block, *refs):
    idx_ref = refs[0]
    xs = refs[1 : 1 + pieces]
    gain_ref, fm_ref, surge_ref, start_ref, wf_hbm, wv_hbm = refs[1 + pieces : 7 + pieces]
    normed_ref, v_ref, k_ref, c_ref, pre_ref, predecay_ref, pack_ref = refs[7 + pieces : 14 + pieces]
    wf, wv, sems = refs[14 + pieces :]
    copies = [
        pltpu.make_async_copy(wf_hbm, wf, sems.at[0]),
        pltpu.make_async_copy(wv_hbm, wv, sems.at[1]),
    ]
    for copy in copies:
        copy.start()
    tokens, width = xs[0].shape
    blocks = tokens // block
    heads = v_ref.shape[1] // DK
    step = block // 4

    def norm_rows(i, _):
        rows = pl.ds(pl.multiple_of(i * step, step), step)
        parts = [x[rows, :].astype(F32) for x in xs]
        total = sum(jnp.sum(part * part, axis=1, keepdims=True) for part in parts)
        scale = lax.rsqrt(total / (width * pieces) + EPS)
        for j, part in enumerate(parts):
            p = idx_ref[j]
            lanes = pl.ds(pl.multiple_of(p * width, 128), width)
            normed_ref[rows, lanes] = (part * scale * gain_ref[p].astype(F32)).astype(BF16)
        return 0

    lax.fori_loop(0, tokens // step, norm_rows, 0)
    for copy in copies:
        copy.wait()
    row = lax.broadcasted_iota(jnp.int32, (block, block), 0)
    col = lax.broadcasted_iota(jnp.int32, (block, block), 1)
    tri = jnp.where(row >= col, 1.0, 0.0).astype(BF16)
    room = 1.0 - fm_ref[...]
    pack_ref[...] = jnp.zeros(pack_ref.shape, BF16)
    pack_ref[:, DV : DV + start_ref.shape[1], :] = start_ref[...].astype(BF16)
    pre_ref[0] = jnp.zeros(pre_ref.shape[1:], F32)
    predecay_ref[0] = jnp.ones(predecay_ref.shape[1:], F32)

    def one_block(b, _):
        rows = pl.ds(pl.multiple_of(b * block, block), block)
        normed = normed_ref[rows, :]
        forget = jnp.dot(normed, wf[...], preferred_element_type=F32).astype(BF16).astype(F32)
        value = jnp.dot(normed, wv[...], preferred_element_type=F32).astype(BF16)
        v_ref[rows, :] = value
        keys = room * jax.nn.sigmoid(-forget)
        k_ref[rows, :] = keys
        log_forget = jnp.log1p(-keys) + surge_ref[rows, :]
        high = log_forget.astype(BF16)
        low = (log_forget - high.astype(F32)).astype(BF16)
        total = jnp.dot(tri, high, preferred_element_type=F32) + jnp.dot(
            tri, low, preferred_element_type=F32
        )
        c_ref[rows, :] = total
        end = total[block - 1 : block, :]
        scaled = (keys * jnp.exp(end - total)).astype(BF16)
        decay = jnp.exp(end)
        after_decay = predecay_ref[b] * decay
        predecay_ref[b + 1] = after_decay
        for h in range(heads):
            span = slice(h * DK, (h + 1) * DK)
            after = decay[:, span] * pre_ref[b, h] + dot_tn(value[:, span], scaled[:, span])
            pre_ref[b + 1, h] = after
        return 0

    lax.fori_loop(0, blocks, one_block, 0)
    last = predecay_ref[blocks]
    last_high = last.astype(BF16)
    last_low = (last - last_high.astype(F32)).astype(BF16)
    for h in range(heads):
        span = slice(h * DK, (h + 1) * DK)
        pack_ref[h, :DV, :] = pre_ref[blocks, h].astype(BF16)
        base = DV + start_ref.shape[1]
        pack_ref[h, base : base + 1, :] = last_high[:, span]
        pack_ref[h, base + 1 : base + 2, :] = last_low[:, span]


def conv_in_kernel(normed_ref, wa_hbm, wb_hbm, mixed_ref, wa, wb, sems):
    copies = [
        pltpu.make_async_copy(wa_hbm, wa, sems.at[0]),
        pltpu.make_async_copy(wb_hbm, wb, sems.at[1]),
    ]
    for copy in copies:
        copy.start()
    for copy in copies:
        copy.wait()
    step = 256

    def rows_of(i, _):
        rows = pl.ds(pl.multiple_of(i * step, step), step)
        normed = normed_ref[rows, :]
        first = jnp.dot(normed, wa[...], preferred_element_type=F32).astype(BF16).astype(F32)
        second = jnp.dot(normed, wb[...], preferred_element_type=F32).astype(BF16).astype(F32)
        mixed_ref[rows, :] = first * second
        return 0

    lax.fori_loop(0, normed_ref.shape[0] // step, rows_of, 0)


def project_kernel(count, *refs):
    normed_ref = refs[0]
    hbm = refs[1 : 1 + count]
    outs = refs[1 + count : 1 + 2 * count]
    bufs = refs[1 + 2 * count : 1 + 3 * count]
    sems = refs[1 + 3 * count]
    copies = [pltpu.make_async_copy(hbm[i], bufs[i], sems.at[i]) for i in range(count)]
    for copy in copies:
        copy.start()
    step = 256
    for i in range(count):
        copies[i].wait()

        def rows_of(r, _):
            rows = pl.ds(pl.multiple_of(r * step, step), step)
            outs[i][rows, :] = jnp.dot(
                normed_ref[rows, :], bufs[i][...], preferred_element_type=F32
            ).astype(BF16)
            return 0

        lax.fori_loop(0, normed_ref.shape[0] // step, rows_of, 0)


def mix_kernel(outputs, ids_ref, *refs):
    (
        q_ref, k_ref, c_ref, v_ref, og_ref, post_ref, mixed_ref, edge_ref, rim_ref, taps_ref,
        hgain_ref, enter_ref, pre_ref, predecay_ref, wr_ref, wc_ref,
    ) = refs[:16]
    outs = refs[16 : 16 + outputs]
    i = pl.program_id(0)
    b = ids_ref[i]
    block, width = q_ref.shape
    heads = width // DK
    sub = block // 4
    row = lax.broadcasted_iota(jnp.int32, (block, block), 0)
    col = lax.broadcasted_iota(jnp.int32, (block, block), 1)
    inner = (row // sub == col // sub) & (row >= col)
    near = (row // (2 * sub) == col // (2 * sub)) & (row // sub > col // sub)
    far = row // (2 * sub) > col // (2 * sub)
    rec = []
    for h in range(heads):
        span = slice(h * DK, (h + 1) * DK)
        q = q_ref[:, span].astype(F32)
        q = q * jax.nn.sigmoid(q) * (DK ** -0.5)
        k = k_ref[:, span]
        c = c_ref[:, span]
        v = v_ref[:, span]
        c4 = c.reshape(4, sub, DK)
        d4 = (c4 - c4[:, sub // 2 : sub // 2 + 1, :]).reshape(block, DK)
        c2 = c.reshape(2, 2 * sub, DK)
        d2 = (c2 - c2[:, sub - 1 : sub, :]).reshape(block, DK)
        d1 = c - c[2 * sub - 1 : 2 * sub, :]
        s4 = dot_nt((q * jnp.exp(d4)).astype(BF16), (k * jnp.exp(-d4)).astype(BF16))
        s2 = dot_nt(
            (q * jnp.exp(jnp.minimum(d2, 0.0))).astype(BF16),
            (k * jnp.exp(jnp.minimum(-d2, 0.0))).astype(BF16),
        )
        s1 = dot_nt(
            (q * jnp.exp(jnp.minimum(d1, 0.0))).astype(BF16),
            (k * jnp.exp(jnp.minimum(-d1, 0.0))).astype(BF16),
        )
        scores = jnp.where(inner, s4, jnp.where(near, s2, jnp.where(far, s1, 0.0)))
        state = pre_ref[0, h] + predecay_ref[0, :, span] * enter_ref[h]
        out = jnp.dot(scores.astype(BF16), v, preferred_element_type=F32) + dot_nt(
            (q * jnp.exp(c)).astype(BF16), state.astype(BF16)
        )
        scale = lax.rsqrt(jnp.mean(out * out, axis=1, keepdims=True) + EPS)
        gate = og_ref[:, span].astype(F32)
        gate = gate * jax.nn.sigmoid(gate)
        rec.append((out * scale * hgain_ref[...].astype(F32) * gate).astype(BF16))
    rec = jnp.concatenate(rec, axis=1)
    mixed = mixed_ref[...]
    edge = jnp.where(b == 0, rim_ref[...], edge_ref[...])
    padded = jnp.concatenate([edge, mixed], axis=0)
    taps = taps_ref[...].astype(F32)
    base = edge.shape[0] - (CK - 1)
    conv = padded[base : base + block] * taps[0:1]
    for j in range(1, CK):
        conv = conv + padded[base + j : base + j + block] * taps[j : j + 1]
    conv = (post_ref[...].astype(F32) * conv).astype(BF16)
    result = (
        jnp.dot(rec, wr_ref[...], preferred_element_type=F32)
        + jnp.dot(conv, wc_ref[...], preferred_element_type=F32)
    ).astype(BF16)
    for n in range(outputs):

        @pl.when(i == n)
        def _():
            outs[n][...] = result


def shards(
    layer_input,
    input_norm_gain,
    query_weight,
    forget_weight,
    value_matrix,
    output_gate_weight,
    after_gate_weight,
    before_gate_weight,
    convolution_input_weight,
    forget_minimum,
    surge_log_decay,
    convolution_kernel,
    head_norm_gain,
    starting_state,
    recurrence_output_weight,
    convolution_output_weight,
    output_norm_gain,
):
    tokens, piece = layer_input.shape
    features, width = query_weight.shape
    heads = width // DK
    tp = lax.axis_size("tp")
    sp = lax.axis_size("sp")
    me = lax.axis_index("tp")
    at = lax.axis_index("sp")
    block = tokens // tp
    blocks = tp

    held = [layer_input]
    order = [0]
    bit = tp // 2
    while bit:
        held = held + [xor_permute(x, "tp", bit) for x in held]
        order = order + [m | bit for m in order]
        bit //= 2
    ids = jnp.stack([me ^ m for m in order]).astype(jnp.int32)

    sds = jax.ShapeDtypeStruct
    krows = starting_state.shape[1]
    pack_rows = DV + krows + 16
    params = pltpu.CompilerParams(vmem_limit_bytes=56 * 1024 * 1024)
    weight_buf = pltpu.VMEM((features, width), BF16)
    normed, value, keys, decay, pre, predecay, pack = pl.pallas_call(
        functools.partial(state_kernel, tp, block),
        out_shape=(
            sds((tokens, features), BF16),
            sds((tokens, width), BF16),
            sds((tokens, width), F32),
            sds((tokens, width), F32),
            sds((blocks + 1, heads, DV, DK), F32),
            sds((blocks + 1, 1, width), F32),
            sds((heads, pack_rows, 128), BF16),
        ),
        in_specs=[SMEM] + [VMEM] * tp + [VMEM] * 4 + [ANY] * 2,
        out_specs=[VMEM] * 7,
        scratch_shapes=[weight_buf, weight_buf, pltpu.SemaphoreType.DMA((2,))],
        compiler_params=params,
        name="state",
    )(
        ids,
        *held,
        input_norm_gain.reshape(tp, 1, piece),
        forget_minimum.reshape(1, width),
        surge_log_decay,
        starting_state,
        forget_weight,
        value_matrix,
    )

    every = lax.all_gather(pack, "sp", axis=0, tiled=False)

    mixed_in = pl.pallas_call(
        conv_in_kernel,
        out_shape=sds((tokens, width), F32),
        in_specs=[VMEM, ANY, ANY],
        out_specs=VMEM,
        scratch_shapes=[weight_buf, weight_buf, pltpu.SemaphoreType.DMA((2,))],
        compiler_params=params,
        name="conv_in",
    )(normed, before_gate_weight, convolution_input_weight)
    rim = from_behind(mixed_in[tokens - 8 :], "sp", 1)
    query, outgate, postgate = pl.pallas_call(
        functools.partial(project_kernel, 3),
        out_shape=[sds((tokens, width), BF16)] * 3,
        in_specs=[VMEM] + [ANY] * 3,
        out_specs=[VMEM] * 3,
        scratch_shapes=[weight_buf] * 3 + [pltpu.SemaphoreType.DMA((3,))],
        compiler_params=params,
        name="project",
    )(normed, query_weight, output_gate_weight, after_gate_weight)

    states = every[:, :, :DV, :].astype(F32)
    totals = jnp.sum(every[:, :, DV + krows : DV + krows + 2, :].astype(F32), axis=2, keepdims=True)
    start = every[:, :, DV : DV + krows, :].astype(F32)
    enter = start.transpose(1, 3, 0, 2).reshape(heads, DV, DK)
    for j in range(sp - 1):
        enter = jnp.where(j < at, totals[j] * enter + states[j], enter)

    half = tp // 2
    rows8 = block // 8

    def mix(block_ids):
        count = len(block_ids)
        at_block = lambda i, ids: (ids[i], 0)
        whole = lambda *shape: pl.BlockSpec(shape, lambda i, ids: (0,) * len(shape))
        tile = pl.BlockSpec((block, width), at_block)
        return pl.pallas_call(
            functools.partial(mix_kernel, count),
            grid_spec=pltpu.PrefetchScalarGridSpec(
                num_scalar_prefetch=1,
                grid=(count,),
                in_specs=[
                    tile, tile, tile, tile, tile, tile, tile,
                    pl.BlockSpec((8, width), lambda i, ids: (jnp.maximum(ids[i] * rows8 - 1, 0), 0)),
                    whole(8, width),
                    whole(CK, width),
                    whole(1, DV),
                    whole(heads, DV, DK),
                    pl.BlockSpec((1, heads, DV, DK), lambda i, ids: (ids[i], 0, 0, 0)),
                    pl.BlockSpec((1, 1, width), lambda i, ids: (ids[i], 0, 0)),
                    whole(width, features),
                    whole(width, features),
                ],
                out_specs=[whole(block, features)] * count,
            ),
            out_shape=[sds((block, features), BF16)] * count,
            compiler_params=params,
            name="mix",
        )(
            jnp.stack(block_ids).astype(jnp.int32),
            query, keys, decay, value, outgate, postgate, mixed_in, mixed_in, rim,
            convolution_kernel, head_norm_gain.reshape(1, DV), enter, pre, predecay,
            recurrence_output_weight, convolution_output_weight,
        )

    def fold(parts):
        parts = list(parts)
        step = len(parts) // 2
        bit = 1
        while step:
            moved = [xor_permute(parts[m], "tp", bit) for m in range(1, len(parts), 2)]
            parts = [
                (parts[2 * n].astype(F32) + moved[n].astype(F32)).astype(BF16)
                for n in range(step)
            ]
            step //= 2
            bit *= 2
        return parts[0]

    away = fold(mix([me ^ (half + m) for m in range(half)]))
    arrived = xor_permute(away, "tp", half)
    home = fold(mix([me ^ m for m in range(half)]))
    mixed = home.astype(F32) + arrived.astype(F32)
    scale = lax.rsqrt(jnp.mean(mixed * mixed, axis=-1, keepdims=True) + EPS)
    return (mixed * scale * output_norm_gain.astype(F32)).astype(BF16)


def solution(mesh):
    return jax.shard_map(
        shards,
        mesh=mesh,
        in_specs=(
            P("sp", "tp"),
            P(),
            P(None, "tp"),
            P(None, "tp"),
            P(None, "tp"),
            P(None, "tp"),
            P(None, "tp"),
            P(None, "tp"),
            P(None, "tp"),
            P("tp"),
            P("sp", "tp"),
            P(None, "tp"),
            P(),
            P("tp", "sp", None),
            P("tp", None),
            P("tp", None),
            P(),
        ),
        out_specs=P(("sp", "tp"), None),
        check_vma=False,
    )
```

```python
import functools

import jax
import jax.numpy as jnp
from jax import lax
from jax.experimental import pallas as pl
from jax.experimental.pallas import tpu as pltpu
from jax.sharding import PartitionSpec as P

DK = 128
DV = 128
CK = 3
EPS = 1e-06
F32 = jnp.float32
BF16 = jnp.bfloat16
ANY = pl.BlockSpec(memory_space=pl.ANY)
SMEM = pl.BlockSpec(memory_space=pltpu.SMEM)


def xor_permute(value, axis, bit):
    peers = lax.axis_size(axis)
    return lax.ppermute(value, axis, [(i, i ^ bit) for i in range(peers)])


def dot_nt(a, b):
    return lax.dot_general(a, b, (((1,), (1,)), ((), ())), preferred_element_type=F32)


def dot_tn(a, b):
    return lax.dot_general(a, b, (((0,), (0,)), ((), ())), preferred_element_type=F32)


class Refs:
    def __init__(self, names, refs):
        self.__dict__.update(zip(names, refs))

    def get(self, name):
        return self.__dict__[name]


def named_call(body, name, ins, outs, scratch, aliases=None):
    names = list(ins) + list(outs) + list(scratch)
    in_names, out_names = list(ins), list(outs)
    aliases = aliases or {}

    def kernel(*refs):
        body(Refs(names, refs))

    results = pl.pallas_call(
        kernel,
        grid=(1,),
        out_shape=[shape for shape, _ in outs.values()],
        in_specs=[spec for _, spec in ins.values()],
        out_specs=[spec for _, spec in outs.values()],
        scratch_shapes=list(scratch.values()),
        input_output_aliases={in_names.index(a): out_names.index(b) for a, b in aliases.items()},
        compiler_params=pltpu.CompilerParams(vmem_limit_bytes=56 * 1024 * 1024),
        name=name,
    )(*[array for array, _ in ins.values()])
    return dict(zip(out_names, results))


def weight_copies(r, weights):
    copies = {}
    for n, w in enumerate(weights):
        copies[w] = pltpu.make_async_copy(r.get("hbm_" + w), r.get("buf_" + w), r.sems.at[n])
        copies[w].start()
    return copies


def norm_piece(r, pieces):
    xs = [r.get("x%d" % j) for j in range(pieces)]
    tokens, width = xs[0].shape
    step = 48

    def norm_rows(i, _):
        rows = pl.ds(pl.multiple_of(i * step, step), step)
        parts = [x[rows, :].astype(F32) for x in xs]
        total = sum(jnp.sum(part * part, axis=1, keepdims=True) for part in parts)
        scale = lax.rsqrt(total / (width * pieces) + EPS)
        for j, part in enumerate(parts):
            p = r.ids[j]
            lanes = pl.ds(pl.multiple_of(p * width, 128), width)
            r.normed[rows, lanes] = (part * scale * r.gain[p].astype(F32)).astype(BF16)
        return 0

    lax.fori_loop(0, tokens // step, norm_rows, 0, unroll=2)


def project(r, copies, w):
    copies[w].wait()
    return jnp.dot(r.normed[...], r.get("buf_" + w)[...], preferred_element_type=F32).astype(BF16)


def forget_value_state(r, copies, block, first, last):
    r.forget[...] = project(r, copies, "forget")
    r.value[...] = project(r, copies, "value")
    tokens, width = r.value.shape
    heads = width // DK
    row = lax.broadcasted_iota(jnp.int32, (block, block), 0)
    col = lax.broadcasted_iota(jnp.int32, (block, block), 1)
    tri = jnp.where(row >= col, 1.0, 0.0).astype(BF16)
    for b in range(tokens // block):
        rows = slice(b * block, (b + 1) * block)
        for h in range(heads):
            span = slice(h * DK, (h + 1) * DK)
            keys = (1.0 - r.minimum[:, span]) * jax.nn.sigmoid(-r.forget[rows, span].astype(F32))
            r.keys[rows, span] = keys
            log_forget = jnp.log1p(-keys) + r.surge[rows, span]
            high = log_forget.astype(BF16)
            low = (log_forget - high.astype(F32)).astype(BF16)
            total = jnp.dot(tri, high, preferred_element_type=F32) + jnp.dot(
                tri, low, preferred_element_type=F32
            )
            r.decay[rows, span] = total
            end = total[block - 1 : block, :]
            scaled = (keys * jnp.exp(end - total)).astype(BF16)
            fade = jnp.exp(end)
            if b == 0 and first:
                before, sofar = jnp.zeros((DV, DK), F32), jnp.ones((1, DK), F32)
            elif b == 0:
                before, sofar = r.carry[h], r.carry_decay[:, span]
            else:
                before, sofar = r.pre[b, h], r.predecay[b, :, span]
            if b == 0:
                r.pre[0, h] = before
                r.predecay[0, :, span] = sofar
            after = fade * before + dot_tn(r.value[rows, span], scaled)
            sofar = sofar * fade
            if (b + 1) * block < tokens:
                r.pre[b + 1, h] = after
                r.predecay[b + 1, :, span] = sofar
            elif not last:
                r.carry_out[h] = after
                r.carry_decay_out[:, span] = sofar
            else:
                peers, _, rows_each, _ = r.pack.shape
                after = after.astype(BF16)
                high = sofar.astype(BF16)
                low = (sofar - high.astype(F32)).astype(BF16)
                for s in range(peers):
                    r.pack[s, h] = after[s * rows_each : (s + 1) * rows_each, :]
                    for part, line in ((high, h), (low, heads + h)):
                        at_row = line % rows_each
                        r.pack[s, heads + line // rows_each, at_row : at_row + 1, :] = part


def advance_kernel(r, heads):
    peers, _, rows_each, _ = r.moved.shape
    for h in range(heads):
        running = r.start[h]
        for s in range(peers):
            r.enter[s, h] = running.astype(BF16)
            total = sum(
                r.moved[s, heads + line // rows_each, line % rows_each : line % rows_each + 1, :].astype(F32)
                for line in (h, heads + h)
            )
            running = total * running + r.moved[s, h].astype(F32)
    edge = r.mixed[r.mixed.shape[0] - (CK - 1) :, :]
    lines = []
    for h in range(edge.shape[1] // DK):
        part = edge[:, h * DK : (h + 1) * DK]
        high = part.astype(BF16).astype(F32)
        lines += [high, part - high]
    lines = jnp.concatenate(lines, axis=0).astype(BF16)
    for n in range(lines.shape[0] // rows_each):
        for s in range(peers):
            r.enter[s, heads + n] = lines[n * rows_each : (n + 1) * rows_each, :]


def mix_kernel(outputs, ids_ref, *refs):
    (
        q_ref, k_ref, c_ref, v_ref, og_ref, post_ref, mixed_ref, edge_ref, taps_ref,
        hgain_ref, enter_ref, pre_ref, predecay_ref, wr_hbm, wc_hbm,
    ) = refs[:15]
    outs = refs[15 : 15 + outputs]
    wr_ref, wc_ref, sems = refs[15 + outputs :]
    i = pl.program_id(0)
    b = ids_ref[i]
    at = ids_ref[outputs]
    copies = [
        pltpu.make_async_copy(wr_hbm, wr_ref, sems.at[0]),
        pltpu.make_async_copy(wc_hbm, wc_ref, sems.at[1]),
    ]

    @pl.when(i == 0)
    def _():
        for copy in copies:
            copy.start()

    block, width = q_ref.shape
    heads = width // DK
    sub = block // 4
    row = lax.broadcasted_iota(jnp.int32, (block, block), 0)
    col = lax.broadcasted_iota(jnp.int32, (block, block), 1)
    inner = (row // sub == col // sub) & (row >= col)
    near = (row // (2 * sub) == col // (2 * sub)) & (row // sub > col // sub)
    far = row // (2 * sub) > col // (2 * sub)
    rec = []
    for h in range(heads):
        span = slice(h * DK, (h + 1) * DK)
        q = q_ref[:, span].astype(F32)
        q = q * jax.nn.sigmoid(q) * (DK ** -0.5)
        k = k_ref[:, span]
        c = c_ref[:, span]
        v = v_ref[:, span]
        c4 = c.reshape(4, sub, DK)
        d4 = (c4 - c4[:, sub // 2 : sub // 2 + 1, :]).reshape(block, DK)
        c2 = c.reshape(2, 2 * sub, DK)
        d2 = (c2 - c2[:, sub - 1 : sub, :]).reshape(block, DK)
        d1 = c - c[2 * sub - 1 : 2 * sub, :]
        s4 = dot_nt((q * jnp.exp(d4)).astype(BF16), (k * jnp.exp(-d4)).astype(BF16))
        s2 = dot_nt(
            (q * jnp.exp(jnp.minimum(d2, 0.0))).astype(BF16),
            (k * jnp.exp(jnp.minimum(-d2, 0.0))).astype(BF16),
        )
        s1 = dot_nt(
            (q * jnp.exp(jnp.minimum(d1, 0.0))).astype(BF16),
            (k * jnp.exp(jnp.minimum(-d1, 0.0))).astype(BF16),
        )
        scores = jnp.where(inner, s4, jnp.where(near, s2, jnp.where(far, s1, 0.0)))
        enter = jnp.concatenate(
            [enter_ref[s, h].astype(F32) for s in range(enter_ref.shape[0])], axis=0
        )
        state = pre_ref[0, h] + predecay_ref[0, :, span] * enter
        out = jnp.dot(scores.astype(BF16), v, preferred_element_type=F32) + dot_nt(
            (q * jnp.exp(c)).astype(BF16), state.astype(BF16)
        )
        scale = lax.rsqrt(jnp.mean(out * out, axis=1, keepdims=True) + EPS)
        gate = og_ref[:, span].astype(F32)
        gate = gate * jax.nn.sigmoid(gate)
        rec.append((out * scale * hgain_ref[...].astype(F32) * gate).astype(BF16))
    rec = jnp.concatenate(rec, axis=1)
    mixed = mixed_ref[...]
    behind = jnp.maximum(at - 1, 0)
    lines = jnp.concatenate(
        [enter_ref[behind, n].astype(F32) for n in range(heads, enter_ref.shape[1])], axis=0
    )
    taken = CK - 1
    rim = jnp.concatenate(
        [
            lines[2 * taken * h : 2 * taken * h + taken] + lines[2 * taken * h + taken : 2 * taken * (h + 1)]
            for h in range(heads)
        ],
        axis=1,
    )
    rim = jnp.concatenate([jnp.zeros((8 - taken, width), F32), rim], axis=0)
    rim = jnp.where(at == 0, 0.0, rim)
    edge = jnp.where(b == 0, rim, edge_ref[...])
    padded = jnp.concatenate([edge, mixed], axis=0)
    taps = taps_ref[...].astype(F32)
    base = edge.shape[0] - (CK - 1)
    conv = padded[base : base + block] * taps[0:1]
    for j in range(1, CK):
        conv = conv + padded[base + j : base + j + block] * taps[j : j + 1]
    conv = (post_ref[...].astype(F32) * conv).astype(BF16)

    @pl.when(i == 0)
    def _():
        for copy in copies:
            copy.wait()

    result = (
        jnp.dot(rec, wr_ref[...], preferred_element_type=F32)
        + jnp.dot(conv, wc_ref[...], preferred_element_type=F32)
    ).astype(BF16)
    for n in range(outputs):

        @pl.when(i == n)
        def _():
            outs[n][...] = result


def shards(
    layer_input,
    input_norm_gain,
    query_weight,
    forget_weight,
    value_matrix,
    output_gate_weight,
    after_gate_weight,
    before_gate_weight,
    convolution_input_weight,
    forget_minimum,
    surge_log_decay,
    convolution_kernel,
    head_norm_gain,
    starting_state,
    recurrence_output_weight,
    convolution_output_weight,
    output_norm_gain,
):
    tokens, piece = layer_input.shape
    features, width = query_weight.shape
    heads = width // DK
    tp = lax.axis_size("tp")
    sp = lax.axis_size("sp")
    me = lax.axis_index("tp")
    at = lax.axis_index("sp")
    block = tokens // tp
    blocks = tp

    chunks = 2
    span = tokens // chunks
    chunk_blocks = span // block
    sds = jax.ShapeDtypeStruct

    parts = [layer_input[n * span : (n + 1) * span] for n in range(chunks)]
    held = [[part] for part in parts]
    order = [0]
    bit = tp // 2
    while bit:
        held = [row + [xor_permute(x, "tp", bit) for x in row] for row in held]
        order = order + [m | bit for m in order]
        bit //= 2
    ids = jnp.stack([me ^ m for m in order]).astype(jnp.int32)

    rows_each = DV // sp
    full_start = lax.all_gather(starting_state, "sp", axis=1, tiled=True)
    start_rows = lax.dynamic_slice_in_dim(full_start, at * rows_each, rows_each, axis=2)
    start_rows = start_rows.transpose(0, 2, 1)

    weights = {
        "forget": forget_weight,
        "value": value_matrix,
        "before": before_gate_weight,
        "convin": convolution_input_weight,
        "query": query_weight,
        "outgate": output_gate_weight,
        "after": after_gate_weight,
    }
    whole = lambda shape: pl.BlockSpec(shape, lambda i: (0,) * len(shape))
    part_of = lambda n, rest: pl.BlockSpec((span, rest), lambda i, n=n: (n, 0))

    def hbm(names):
        return {"hbm_" + w: (weights[w], ANY) for w in names}

    def bufs(names):
        spaces = {"buf_" + w: pltpu.VMEM((features, width), BF16) for w in names}
        spaces["sems"] = pltpu.SemaphoreType.DMA((len(names),))
        return spaces

    def norm_inputs(n):
        taken = {"ids": (ids, SMEM)}
        for j, x in enumerate(held[n]):
            taken["x%d" % j] = (x, whole((span, piece)))
        taken["gain"] = (input_norm_gain.reshape(tp, 1, piece), whole((tp, 1, piece)))
        taken["minimum"] = (forget_minimum.reshape(1, width), whole((1, width)))
        taken["surge"] = (surge_log_decay, part_of(n, width))
        return taken

    def outputs_of(n, names):
        return {
            w: (sds((tokens, width), F32 if w in ("keys", "decay", "mixed") else BF16), part_of(n, width))
            for w in names
        }

    def state_outputs(n):
        taken = outputs_of(n, ("value", "keys", "decay"))
        taken["pre"] = (
            sds((blocks, heads, DV, DK), F32),
            pl.BlockSpec((chunk_blocks, heads, DV, DK), lambda i: (n, 0, 0, 0)),
        )
        taken["predecay"] = (
            sds((blocks, 1, width), F32),
            pl.BlockSpec((chunk_blocks, 1, width), lambda i: (n, 0, 0)),
        )
        return taken

    def before_and_convin(r, copies):
        r.mixed[...] = project(r, copies, "before").astype(F32)
        r.mixed[...] = r.mixed[...] * project(r, copies, "convin").astype(F32)

    def first_body(r):
        copies = weight_copies(r, weights)
        norm_piece(r, tp)
        forget_value_state(r, copies, block, True, False)
        before_and_convin(r, copies)
        for w in ("query", "outgate", "after"):
            r.get(w)[...] = project(r, copies, w)

    full = named_call(
        first_body,
        "first",
        {**norm_inputs(0), **hbm(weights)},
        {
            **state_outputs(0),
            **outputs_of(0, ("mixed", "query", "outgate", "after")),
            "carry_out": (sds((heads, DV, DK), F32), whole((heads, DV, DK))),
            "carry_decay_out": (sds((1, width), F32), whole((1, width))),
        },
        {
            **bufs(weights),
            "normed": pltpu.VMEM((span, features), BF16),
            "forget": pltpu.VMEM((span, width), BF16),
        },
    )

    def second_body(r):
        copies = weight_copies(r, ("forget", "value"))
        norm_piece(r, tp)
        forget_value_state(r, copies, block, False, True)

    slabs = heads + -(-2 * heads // rows_each)
    kept = ("value", "keys", "decay", "pre", "predecay")
    second = named_call(
        second_body,
        "second",
        {
            **norm_inputs(1),
            **hbm(("forget", "value")),
            "carry": (full["carry_out"], whole((heads, DV, DK))),
            "carry_decay": (full["carry_decay_out"], whole((1, width))),
            **{"old_" + w: (full[w], ANY) for w in kept},
        },
        {
            **state_outputs(1),
            "pack": (sds((sp, slabs, rows_each, DK), BF16), whole((sp, slabs, rows_each, DK))),
            "normed": (sds((span, features), BF16), whole((span, features))),
        },
        {**bufs(("forget", "value")), "forget": pltpu.VMEM((span, width), BF16)},
        {"old_" + w: w for w in kept},
    )
    full.update({w: second[w] for w in kept})
    normed = second["normed"]
    moved = lax.all_to_all(second["pack"], "sp", split_axis=0, concat_axis=0, tiled=True)

    def mixed_body(r):
        before_and_convin(r, weight_copies(r, ("before", "convin")))

    full["mixed"] = named_call(
        mixed_body,
        "convin",
        {
            "normed": (normed, whole((span, features))),
            **hbm(("before", "convin")),
            "old_mixed": (full["mixed"], ANY),
        },
        outputs_of(1, ("mixed",)),
        bufs(("before", "convin")),
        {"old_mixed": "mixed"},
    )["mixed"]

    extra = -(-2 * (CK - 1) * heads // rows_each)
    enter = named_call(
        functools.partial(advance_kernel, heads=heads),
        "advance",
        {
            "moved": (moved, whole((sp, slabs, rows_each, DK))),
            "start": (start_rows, whole((heads, rows_each, DK))),
            "mixed": (full["mixed"], pl.BlockSpec((8, width), lambda i: (tokens // 8 - 1, 0))),
        },
        {
            "enter": (
                sds((sp, heads + extra, rows_each, DK), BF16),
                whole((sp, heads + extra, rows_each, DK)),
            )
        },
        {},
    )["enter"]
    normed, enter = lax.optimization_barrier((normed, enter))
    enter = lax.all_to_all(enter, "sp", split_axis=0, concat_axis=0, tiled=True)

    def rest_body(r):
        copies = weight_copies(r, ("query", "outgate", "after"))
        for w in ("query", "outgate", "after"):
            r.get(w)[...] = project(r, copies, w)

    rest = ("query", "outgate", "after")
    full.update(
        named_call(
            rest_body,
            "rest",
            {
                "normed": (normed, whole((span, features))),
                **hbm(rest),
                **{"old_" + w: (full[w], ANY) for w in rest},
            },
            outputs_of(1, rest),
            bufs(rest),
            {"old_" + w: w for w in rest},
        )
    )

    half = tp // 2
    rows8 = block // 8

    def mix(block_ids):
        count = len(block_ids)
        at_block = lambda i, ids: (ids[i], 0)
        whole = lambda *shape: pl.BlockSpec(shape, lambda i, ids: (0,) * len(shape))
        tile = pl.BlockSpec((block, width), at_block)
        return pl.pallas_call(
            functools.partial(mix_kernel, count),
            grid_spec=pltpu.PrefetchScalarGridSpec(
                num_scalar_prefetch=1,
                grid=(count,),
                in_specs=[
                    tile, tile, tile, tile, tile, tile, tile,
                    pl.BlockSpec((8, width), lambda i, ids: (jnp.maximum(ids[i] * rows8 - 1, 0), 0)),
                    whole(CK, width),
                    whole(1, DV),
                    whole(sp, heads + extra, rows_each, DK),
                    pl.BlockSpec((1, heads, DV, DK), lambda i, ids: (ids[i], 0, 0, 0)),
                    pl.BlockSpec((1, 1, width), lambda i, ids: (ids[i], 0, 0)),
                    ANY,
                    ANY,
                ],
                scratch_shapes=[
                    pltpu.VMEM((width, features), BF16),
                    pltpu.VMEM((width, features), BF16),
                    pltpu.SemaphoreType.DMA((2,)),
                ],
                out_specs=[whole(block, features)] * count,
            ),
            out_shape=[sds((block, features), BF16)] * count,
            compiler_params=pltpu.CompilerParams(vmem_limit_bytes=56 * 1024 * 1024),
            name="mix",
        )(
            jnp.stack(list(block_ids) + [at]).astype(jnp.int32),
            full["query"], full["keys"], full["decay"], full["value"], full["outgate"],
            full["after"], full["mixed"], full["mixed"],
            convolution_kernel, head_norm_gain.reshape(1, DV), enter, full["pre"], full["predecay"],
            recurrence_output_weight, convolution_output_weight,
        )

    def fold(parts):
        parts = list(parts)
        step = len(parts) // 2
        bit = 1
        while step:
            moved = [xor_permute(parts[m], "tp", bit) for m in range(1, len(parts), 2)]
            parts = [
                (parts[2 * n].astype(F32) + moved[n].astype(F32)).astype(BF16)
                for n in range(step)
            ]
            step //= 2
            bit *= 2
        return parts[0]

    away = fold(mix([me ^ (half + m) for m in range(half)]))
    away, later = lax.optimization_barrier((away, me))
    arrived = xor_permute(away, "tp", half)
    home = fold(mix([later ^ m for m in range(half)]))
    mixed = home.astype(F32) + arrived.astype(F32)
    scale = lax.rsqrt(jnp.mean(mixed * mixed, axis=-1, keepdims=True) + EPS)
    return (mixed * scale * output_norm_gain.astype(F32)).astype(BF16)


def solution(mesh):
    return jax.shard_map(
        shards,
        mesh=mesh,
        in_specs=(
            P("sp", "tp"),
            P(),
            P(None, "tp"),
            P(None, "tp"),
            P(None, "tp"),
            P(None, "tp"),
            P(None, "tp"),
            P(None, "tp"),
            P(None, "tp"),
            P("tp"),
            P("sp", "tp"),
            P(None, "tp"),
            P(),
            P("tp", "sp", None),
            P("tp", None),
            P("tp", None),
            P(),
        ),
        out_specs=P(("sp", "tp"), None),
        check_vma=False,
    )
```
